1024 devices in a mesh: row: 64 (over z, core), col: 16 (over y, x).
Axes of the slice: x: 4, y: 4, z: 32, core: 2. Of those that a mesh axis runs over, the one named last changes fastest.
Arguments:
- streams: bfloat16 [3, 1, 131072, 512], P(None, None, ('row', 'col')), may hold values from -6 to 6
- filter_taps: float32 [2, 131072, 512], P(None, ('row', 'col')), may hold values from -4 to 4
- short_taps: float32 [3, 3, 512], replicated, may hold values from -3 to 3
- skip_gain: float32 [512], replicated, may hold values from -3 to 3
- out_weight: bfloat16 [512, 4096], replicated, may hold values from -0.25 to 0.25
Outputs:
- projected: bfloat16 [1, 131072, 4096], P(None, ('row', 'col'))
The draws below stay inside these ranges and needn't reach their ends.
All inputs are finite; a program needn't handle non-finite values.
Results may differ from the reference program's by a relative error of at most 0.0049.
Values may be sent and summed in bfloat16 or wider, within the bound.
A program may use at most 32 MiB of HBM per device.

```python
import math
import jax
import jax.numpy as jnp
from jax import lax

WIDTH = 4096
CHANNELS = 512
SEQUENCES = 1
LENGTH = 131072


def draw_filter_taps(key, part):
    subkeys = jax.random.split(jax.random.fold_in(key, 11), 4)
    roughness = jax.random.truncated_normal(subkeys[0], -4.0, 4.0, (2, LENGTH, CHANNELS), jnp.float32)
    selector = jax.random.uniform(subkeys[1], (2, 1, CHANNELS), jnp.float32)
    slow_reach = LENGTH * jnp.exp(jax.random.uniform(subkeys[2], (2, 1, CHANNELS), jnp.float32, math.log(0.5), math.log(4.0)))
    fast_reach = jnp.exp(jax.random.uniform(subkeys[3], (2, 1, CHANNELS), jnp.float32, math.log(30.0), math.log(50.0)))
    share_slow = 0.5
    chosen_reach = jnp.where(selector < share_slow, slow_reach, fast_reach)
    offsets = jnp.arange(LENGTH, dtype=jnp.float32)
    distance = jnp.stack([offsets, LENGTH - offsets])[:, :, None]
    envelope = jnp.exp(-distance / chosen_reach)
    magnitude = jnp.sqrt(jnp.sum(jnp.square(envelope), axis=(0, 1), keepdims=True))
    return roughness * envelope / magnitude


def steps_of(key, dims, shards, smallest, largest):
    def one(position, shards_of):
        steps = jax.random.uniform(jax.random.fold_in(jax.random.fold_in(key, 6), position), (shards_of,), jnp.float32, smallest / len(shards), largest / len(shards))
        return jnp.repeat(jnp.exp(steps), dims[position] // shards_of).reshape((-1,) + (1,) * (len(dims) - position - 1))

    level = one(*shards[0])
    for cut in shards[1:]:
        level = level * one(*cut)
    return level


def normal_values(stream_key, shape, deviation, most, cuts=(), kind=jnp.bfloat16):
    array = jax.random.normal(stream_key, shape, jnp.float32) * deviation
    if len(cuts) > 0:
        array = steps_of(stream_key, shape, cuts, -0.22, 0.18) * array
    return jnp.clip(array, min=-most, max=most).astype(kind)


def setup_inputs(seed: int = 0) -> dict:
    seeds = jax.random.split(jax.random.key(seed), 6)
    streams = normal_values(seeds[0], (3, SEQUENCES, LENGTH, CHANNELS), 1.0, 6.0, ((2, 1024),))
    filter_taps = draw_filter_taps(jax.random.fold_in(seeds[5], 71), 0)
    short_taps = normal_values(seeds[2], (3, 3, CHANNELS), 0.577, 3.0, (), jnp.float32)
    skip_gain = normal_values(seeds[3], (CHANNELS,), 0.5, 3.0, (), jnp.float32)
    out_weight = normal_values(seeds[4], (CHANNELS, WIDTH), CHANNELS ** -0.5, 0.25)
    return {"streams": streams, "filter_taps": filter_taps, "short_taps": short_taps, "skip_gain": skip_gain, "out_weight": out_weight}


EPSILON = 1e-06

def smooth_streams(streams, short_taps):
    widened = streams.astype(jnp.float32)
    padded = jnp.pad(widened, ((0, 0), (0, 0), (1, 1), (0, 0)))
    return short_taps[:, 0][:, None, None, :] * padded[:, :, :-2] + short_taps[:, 1][:, None, None, :] * padded[:, :, 1:-1] + short_taps[:, 2][:, None, None, :] * padded[:, :, 2:]

def reference(streams, filter_taps, short_taps, skip_gain, out_weight):
    smoothed = smooth_streams(streams, short_taps)
    gated = smoothed[2] * smoothed[1]
    kernel_spectrum = jnp.fft.rfft(filter_taps.reshape(2 * LENGTH, CHANNELS), axis=0)

    def one_sequence(operands):
        gated_rows, gate_rows = operands
        spectrum = jnp.fft.rfft(gated_rows, n=2 * LENGTH, axis=0) * kernel_spectrum
        convolved = jnp.fft.irfft(spectrum, n=2 * LENGTH, axis=0)[:LENGTH]
        mixed = ((convolved + skip_gain * gated_rows) * gate_rows).astype(jnp.bfloat16)
        mean_square = lax.optimization_barrier(jnp.mean(jnp.square(mixed.astype(jnp.float32)), axis=-1, keepdims=True))
        product = jnp.dot(mixed, out_weight, preferred_element_type=jnp.float32)
        return (product * lax.rsqrt(mean_square + EPSILON)).astype(jnp.bfloat16)
    return lax.map(one_sequence, (gated, smoothed[0]))
```

```python
import math

import jax
import jax.numpy as jnp
import numpy as np
from jax import lax
from jax.sharding import PartitionSpec as P

EPSILON = 1e-06
HIGH = lax.Precision.HIGH


def tables():
    s = np.arange(1024, dtype=np.int64)
    q = np.arange(1024, dtype=np.int64)
    j = np.arange(128, dtype=np.int64)
    ang = np.pi * ((2 * q[:, None] + 1) * s[None] % 4096) / 2048.0
    m1 = np.stack([np.cos(ang), -np.sin(ang)]).reshape(2, 2, 512, 1024).transpose(1, 0, 2, 3).reshape(2, 1024, 1024)
    ang = np.pi * ((2 * q[:, None] + 1) * j[None]) / 262144.0
    tw = np.stack([np.cos(ang), -np.sin(ang)]).reshape(2, 2, 512, 128).transpose(1, 0, 2, 3)
    ang = 2 * np.pi * (j[:, None] * j[None] % 128) / 128.0
    c, n = np.cos(ang), np.sin(ang)
    fwd = np.block([[c, -n], [n, c]])
    inv = np.block([[c, n], [-n, c]])
    return m1, tw, fwd, inv


def halo(streams):
    size = 1024
    axes = ("row", "col")
    up = [(i, i + 1) for i in range(size - 1)]
    low = lax.ppermute(streams[:, :, -1:], axes, up)
    high = lax.ppermute(streams[:, :, :1], axes, [(b, a) for a, b in up])
    return jnp.concatenate([low, streams, high], axis=2)


def local(streams, filter_taps, short_taps, skip_gain, out_weight):
    m1, tw, fwd, inv = tables()
    core = lax.axis_index("row") % 2
    m1 = jnp.asarray(m1, jnp.bfloat16)[core]
    tw = jnp.asarray(tw, jnp.float32)[core]
    fwd = jnp.asarray(fwd, jnp.float32)
    inv = jnp.asarray(inv, jnp.float32)
    padded = halo(streams)
    smoothed = (
        short_taps[:, 0][:, None, None, :] * padded[:, :, :-2]
        + short_taps[:, 1][:, None, None, :] * padded[:, :, 1:-1]
        + short_taps[:, 2][:, None, None, :] * padded[:, :, 2:]
    )[:, 0]
    gated = smoothed[2] * smoothed[1]
    data = jnp.concatenate([gated[None].astype(jnp.bfloat16), filter_taps.astype(jnp.bfloat16)], axis=0)
    data = jnp.swapaxes(data, 1, 2)
    data = lax.all_to_all(data.reshape(3, 16, 32, 128), "col", split_axis=1, concat_axis=1, tiled=True)
    data = jnp.transpose(data, (2, 0, 1, 3))
    zgroups = [[2 * z + k for z in range(32)] for k in range(2)]
    pairs = [[2 * z, 2 * z + 1] for z in range(32)]
    data = lax.all_to_all(data, "row", split_axis=0, concat_axis=0, axis_index_groups=zgroups, tiled=True)
    data = lax.all_gather(data, "row", axis_index_groups=pairs)
    data = jnp.transpose(data, (2, 1, 0, 3, 4)).reshape(3, 1024, 128)
    spec = jnp.einsum("qs,asj->aqj", m1, data, preferred_element_type=jnp.float32)
    re, im = spec[:, :512], spec[:, 512:]
    sign = (1.0 - 2.0 * (jnp.arange(512) % 2)).astype(jnp.float32)[:, None]
    hre = re[1] - sign * im[2]
    him = im[1] + sign * re[2]

    def rows(re, im):
        both = jnp.concatenate([re * tw[0] - im * tw[1], re * tw[1] + im * tw[0]], axis=1)
        out = jnp.dot(both, fwd, precision=HIGH)
        return out[:, :128], out[:, 128:]

    gre, gim = rows(re[0], im[0])
    hre, him = rows(hre, him)
    both = jnp.concatenate([gre * hre - gim * him, gre * him + gim * hre], axis=1)
    back = jnp.dot(both, inv, precision=HIGH)
    bre, bim = back[:, :128], back[:, 128:]
    both = jnp.concatenate([bre * tw[0] + bim * tw[1], bim * tw[0] - bre * tw[1]], axis=0) * (2.0 ** -17)
    hi = both.astype(jnp.bfloat16)
    lo = (both - hi.astype(jnp.float32)).astype(jnp.bfloat16)
    y = lax.dot_general(m1, jnp.concatenate([hi, lo], axis=1), (((0,), (0,)), ((), ())), preferred_element_type=jnp.float32)
    y = (y[:, :128] + y[:, 128:]).reshape(32, 2, 16, 128)
    mine = jnp.where(core == 0, y[:, 0], y[:, 1])
    other = jnp.where(core == 0, y[:, 1], y[:, 0])
    swap = [(i, i ^ 1) for i in range(64)]
    y = (mine + lax.ppermute(other, "row", swap)).astype(jnp.bfloat16)
    y = lax.all_to_all(y, "row", split_axis=0, concat_axis=0, axis_index_groups=zgroups, tiled=True)
    y = jnp.transpose(y, (1, 0, 2))
    y = lax.all_to_all(y, "col", split_axis=0, concat_axis=0, tiled=True)
    convolved = y.reshape(512, 128).T.astype(jnp.float32)
    mixed = ((convolved + skip_gain * gated) * smoothed[0]).astype(jnp.bfloat16)
    mean_square = jnp.mean(jnp.square(mixed.astype(jnp.float32)), axis=-1, keepdims=True)
    product = jnp.dot(mixed, out_weight, preferred_element_type=jnp.float32)
    return (product * lax.rsqrt(mean_square + EPSILON)).astype(jnp.bfloat16)[None]


def solution(mesh):
    in_specs = (P(None, None, ("row", "col"), None), P(None, ("row", "col"), None), P(), P(), P())
    return jax.shard_map(local, mesh=mesh, in_specs=in_specs, out_specs=P(None, ("row", "col"), None), check_vma=False)
```

```python
import functools

import jax
import jax.numpy as jnp
import numpy as np
from jax import lax
from jax.experimental import pallas as pl
from jax.experimental.pallas import tpu as pltpu
from jax.sharding import PartitionSpec as P

EPSILON = 1e-06
F32 = jnp.float32
BF16 = jnp.bfloat16
MESH = pl.DeviceIdType.MESH


def tables(freqs, length):
    q = np.arange(freqs, dtype=np.int64)[:, None]
    lane = np.arange(128, dtype=np.int64)[None]

    def circle(numerator, period):
        angles = 2.0 * np.pi * (numerator % period) / period
        return [np.cos(angles), -np.sin(angles)]

    twist = circle((2 * q + 1) * lane, 2 * length)
    fine = circle((2 * q + 1) * lane, 4 * freqs)
    coarse = circle((2 * q + 1) * lane * 128, 4 * freqs)
    tabs = np.stack(twist + fine + coarse).reshape(6, 2, freqs // 2, 128).transpose(1, 0, 2, 3)
    cos, sin = circle(lane.T * lane, 128)
    forward = np.block([[cos, sin], [-sin, cos]])
    back = np.block([[cos, -sin], [sin, cos]])
    pair = np.stack([forward, back])
    high = pair.astype(jnp.bfloat16)
    low = (pair - high.astype(np.float64)).astype(jnp.bfloat16)
    return tabs.astype(np.float32), np.stack([high, low], axis=1)


def dot(a, b):
    return jnp.dot(a, b, preferred_element_type=F32)


def split(x):
    high = x.astype(BF16)
    return high, (x - high.astype(F32)).astype(BF16)


def dot3(x, matrix):
    high, low = split(x)
    return dot(high, matrix[0]) + dot(low, matrix[0]) + dot(high, matrix[1])


def kernel(Z, C, taps_w, skip, streams_h, filt_h, tabs_h, dft_h, out,
           st, ft, tb, df, he, hr, sm0, sg, gt, fx, fr, gx, gr, tmpf, tmps, zf, zs, xf, xs,
           m1h, m1l, m2, hs, dc, yo, yr, zo, ro, tmpo, xo, rx,
           load, halo_s, halo_r, send, recv):
    J = 128
    CH = Z * C
    S = 2 * CH
    QH = S // 2
    QB = min(256, QH)
    GB = min(128, QH)
    SB = min(128, S)
    ZP, CP = Z + 8, C + 8
    row, col = lax.axis_index("row"), lax.axis_index("col")
    z, core = row // 2, row % 2
    mate = (z * 2 + 1 - core, col)
    block, blocks = row * C + col, 2 * Z * C
    after, before = (block + 1) % blocks, (block + blocks - 1) % blocks
    after_id, before_id = (after // C, after % C), (before // C, before % C)

    loads = [
        pltpu.make_async_copy(streams_h, st, load.at[0]),
        pltpu.make_async_copy(filt_h, ft, load.at[1]),
        pltpu.make_async_copy(tabs_h.at[core], tb, load.at[2]),
        pltpu.make_async_copy(dft_h, df, load.at[3]),
    ]
    for c in loads:
        c.start()

    def z_at(i):
        return (z + Z // 2 + ((i + 1) // 2) * (1 - 2 * (i % 2))) % Z

    def c_at(i):
        return (col + 1 + i) % C

    barrier = pltpu.get_barrier_semaphore()

    def greet_z(i, carry):
        pl.semaphore_signal(barrier, inc=1, device_id=(z_at(i) * 2 + core, col), device_id_type=MESH)
        return carry

    def greet_c(i, carry):
        pl.semaphore_signal(barrier, inc=1, device_id=(row, c_at(i)), device_id_type=MESH)
        return carry

    lax.fori_loop(0, Z - 1, greet_z, 0)
    lax.fori_loop(0, C - 1, greet_c, 0)
    for d in (mate, after_id, before_id):
        pl.semaphore_signal(barrier, inc=1, device_id=d, device_id_type=MESH)

    def to_z(src, dst, k):
        def body(i, carry):
            t = z_at(i)
            pltpu.make_async_remote_copy(
                src_ref=src.at[t], dst_ref=dst, send_sem=send.at[k], recv_sem=recv.at[k],
                device_id=(t * 2 + core, col), device_id_type=MESH).start()
            return carry
        lax.fori_loop(0, Z - 1, body, 0)

    def to_c(src, dst, k):
        def body(i, carry):
            t = c_at(i)
            pltpu.make_async_remote_copy(
                src_ref=src.at[t], dst_ref=dst, send_sem=send.at[k], recv_sem=recv.at[k],
                device_id=(row, t), device_id_type=MESH).start()
            return carry
        lax.fori_loop(0, C - 1, body, 0)

    def await_all(ref, sem):
        pltpu.make_async_copy(ref, ref, sem).wait()

    loads[1].wait()
    for h in range(2):
        fx[:, h] = ft[h].T.astype(BF16).reshape(C, Z, J)
    fr[col] = fx[col]
    loads[0].wait()
    he[...] = jnp.zeros_like(he)
    for i in range(3):
        x = st[i].astype(F32)
        he[0, i:i + 1] = x[J - 1:J]
        he[1, i:i + 1] = x[0:1]

    pl.semaphore_wait(barrier, Z - 1 + C - 1 + 3)

    halos = [
        pltpu.make_async_remote_copy(src_ref=he.at[k], dst_ref=hr.at[k], send_sem=halo_s.at[k],
                                     recv_sem=halo_r.at[k], device_id=d, device_id_type=MESH)
        for k, d in ((0, after_id), (1, before_id))
    ]
    for c in halos:
        c.start()
    to_c(fx, fr.at[col], 0)
    for c in halos:
        c.wait_recv()
    at = lax.broadcasted_iota(jnp.int32, (J, CH), 0)
    smoothed = []
    for i in range(3):
        x = st[i].astype(F32)
        low = jnp.where(block == 0, 0.0, hr[0, i:i + 1])
        high = jnp.where(block == blocks - 1, 0.0, hr[1, i:i + 1])
        low = jnp.where(at == 0, low, pltpu.roll(x, 1, 0))
        high = jnp.where(at == J - 1, high, pltpu.roll(x, J - 1, 0))
        smoothed.append(taps_w[i, 0:1] * low + taps_w[i, 1:2] * x + taps_w[i, 2:3] * high)
    gated = smoothed[2] * smoothed[1]
    gx[...] = gated.T.astype(BF16).reshape(C, Z, J)
    sm0[...] = smoothed[0]
    sg[...] = skip[...] * gated
    gr[col] = gx[col]
    to_c(gx, gr.at[col], 1)

    await_all(fr.at[pl.ds(0, C - 1)], recv.at[0])
    for h in range(2):
        for c in range(C):
            tmpf[h, c * ZP:c * ZP + Z] = fr[c, h].astype(F32)
    for h in range(2):
        for t in range(Z):
            zf[t, h] = tmpf[h, pl.ds(t, C, stride=ZP), :].astype(BF16)
    to_z(zf, xf.at[z, core], 2)
    xf[z, core] = zf[z]
    await_all(gr.at[pl.ds(0, C - 1)], recv.at[1])
    for c in range(C):
        tmps[c * ZP:c * ZP + Z] = gr[c].astype(F32)
    for t in range(Z):
        zs[t] = tmps[pl.ds(t, C, stride=ZP), :].astype(BF16)
    to_z(zs, xs.at[z, core], 3)
    xs[z, core] = zs[z]

    loads[2].wait()
    loads[3].wait()

    def build(g, carry):
        rows = pl.ds(pl.multiple_of(g * GB, GB), GB)
        fine_re, fine_im = tb[2, rows, 0:SB], tb[3, rows, 0:SB]
        for a in range(S // SB):
            coarse_re, coarse_im = tb[4, rows, a:a + 1], tb[5, rows, a:a + 1]
            parts = (coarse_re * fine_re - coarse_im * fine_im, coarse_re * fine_im + coarse_im * fine_re)
            for k, part in enumerate(parts):
                high, low = split(part)
                per = QB // GB
                where = pl.ds(pl.multiple_of((g % per) * GB, GB) + k * QB, GB)
                m1h[g // per, where, a * SB:(a + 1) * SB] = high
                m1l[g // per, where, a * SB:(a + 1) * SB] = low
                flipped = part.T.astype(BF16)
                for n in range(SB // C):
                    tile = a * (SB // C) + n
                    m2[tile % 2, (tile // 2) * C:(tile // 2 + 1) * C, pl.ds(pl.multiple_of(g * GB, GB) + k * QH, GB)] = (
                        flipped[n * C:(n + 1) * C])
        return carry

    lax.fori_loop(0, QH // GB, build, 0)

    def to_mate(src, dst, k):
        pltpu.make_async_remote_copy(
            src_ref=src, dst_ref=dst, send_sem=send.at[k], recv_sem=recv.at[k],
            device_id=mate, device_id_type=MESH).start()

    def twisted(re, im, rows, sign):
        tw_re, tw_im = tb[0, rows], sign * tb[1, rows]
        return re * tw_re - im * tw_im, re * tw_im + im * tw_re

    await_all(xf.at[pl.ds(0, Z - 1), 0], recv.at[2])
    to_mate(xf.at[:, core], xf.at[:, core], 4)
    await_all(xf.at[:, 0], recv.at[4])

    def filter_rows(b, carry):
        rows = pl.ds(pl.multiple_of(b * QB, QB), QB)
        taps = jnp.concatenate([xf[:, :, h].reshape(S, J) for h in range(2)], axis=1)
        p = dot(m1h[b], taps) + dot(m1l[b], taps)
        sign = 1.0 - 2.0 * (lax.broadcasted_iota(jnp.int32, (QB, J), 0) % 2).astype(F32)
        re = p[:QB, :J] - sign * p[QB:, J:]
        im = p[QB:, :J] + sign * p[:QB, J:]
        hs[rows] = dot3(jnp.concatenate(twisted(re, im, rows, 1.0), axis=1), df[0])
        return carry

    lax.fori_loop(0, QH // QB, filter_rows, 0)

    await_all(xs.at[pl.ds(0, Z - 1), 0], recv.at[3])
    to_mate(xs.at[:, core], xs.at[:, core], 5)
    await_all(xs.at[:, 0], recv.at[5])

    def signal_rows(b, carry):
        rows = pl.ds(pl.multiple_of(b * QB, QB), QB)
        p = dot(m1h[b], xs[...].reshape(S, J))
        g = dot3(jnp.concatenate(twisted(p[:QB], p[QB:], rows, 1.0), axis=1), df[0])
        h = hs[rows]
        gre, gim, hre, him = g[:, :J], g[:, J:], h[:, :J], h[:, J:]
        y = dot3(jnp.concatenate([gre * hre - gim * him, gre * him + gim * hre], axis=1), df[1])
        parts = twisted(y[:, :J], y[:, J:], rows, -1.0)
        for k, part in enumerate(parts):
            high, low = split(part * (1.0 / (S * J)))
            where = pl.ds(pl.multiple_of(b * QB, QB) + k * QH, QB)
            dc[where, 0:J] = high
            dc[where, J:2 * J] = low
        return carry

    lax.fori_loop(0, QH // QB, signal_rows, 0)
    other = dot(m2[1 - core], dc[...])
    yo[...] = (other[:, :J] + other[:, J:]).reshape(Z, C, J)
    to_mate(yo, yr, 6)
    own = dot(m2[core], dc[...])
    own = (own[:, :J] + own[:, J:]).reshape(Z, C, J)
    await_all(yr, recv.at[6])
    zo[...] = (own + yr[...]).astype(BF16)
    to_z(zo, ro.at[z], 7)
    ro[z] = zo[z]
    await_all(ro.at[pl.ds(0, Z - 1)], recv.at[7])
    for t in range(Z):
        tmpo[t * CP:t * CP + C] = ro[t].astype(F32)
    for c in range(C):
        xo[c] = tmpo[pl.ds(c, Z, stride=CP), :].astype(BF16)
    to_c(xo, rx.at[col], 8)
    rx[col] = xo[col]
    await_all(rx.at[pl.ds(0, C - 1)], recv.at[8])
    convolved = rx[...].reshape(CH, J).astype(F32).T
    out[...] = ((convolved + sg[...]) * sm0[...]).astype(BF16)

    for c in halos:
        c.wait_send()
    for ref, k in ((fx.at[pl.ds(0, C - 1)], 0), (gx.at[pl.ds(0, C - 1)], 1), (zf.at[pl.ds(0, Z - 1)], 2),
                   (zs.at[pl.ds(0, Z - 1)], 3), (xf.at[:, 0], 4), (xs.at[:, 0], 5), (yo, 6),
                   (zo.at[pl.ds(0, Z - 1)], 7), (xo.at[pl.ds(0, C - 1)], 8)):
        await_all(ref, send.at[k])


def convolve(Z, C, streams, filter_taps, short_taps, skip_gain):
    J, CH = 128, Z * C
    S = 2 * CH
    QH = S // 2
    QB = min(256, QH)
    tabs, dfts = tables(S, 2 * S * J)
    vmem = pltpu.VMEM
    scratch = [
        vmem((3, J, CH), BF16),
        vmem((2, J, CH), F32),
        vmem((6, QH, 128), F32),
        vmem((2, 2, 2 * J, 2 * J), BF16),
        vmem((2, 8, CH), F32),
        vmem((2, 8, CH), F32),
        vmem((J, CH), F32),
        vmem((J, CH), F32),
        vmem((8, 128), F32),
        vmem((C, 2, Z, J), BF16),
        vmem((C, 2, Z, J), BF16),
        vmem((C, Z, J), BF16),
        vmem((C, Z, J), BF16),
        vmem((2, C * (Z + 8), J), F32),
        vmem((C * (Z + 8), J), F32),
        vmem((Z, 2, C, J), BF16),
        vmem((Z, C, J), BF16),
        vmem((Z, 2, 2, C, J), BF16),
        vmem((Z, 2, C, J), BF16),
        vmem((QH // QB, 2 * QB, S), BF16),
        vmem((QH // QB, 2 * QB, S), BF16),
        vmem((2, S // 2, 2 * QH), BF16),
        vmem((QH, 2 * J), F32),
        vmem((2 * QH, 2 * J), BF16),
        vmem((Z, C, J), F32),
        vmem((Z, C, J), F32),
        vmem((Z, C, J), BF16),
        vmem((Z, C, J), BF16),
        vmem((Z * (C + 8), J), F32),
        vmem((C, Z, J), BF16),
        vmem((C, Z, J), BF16),
        pltpu.SemaphoreType.DMA((4,)),
        pltpu.SemaphoreType.DMA((2,)),
        pltpu.SemaphoreType.DMA((2,)),
        pltpu.SemaphoreType.DMA((9,)),
        pltpu.SemaphoreType.DMA((9,)),
    ]
    inside, outside = pl.BlockSpec(memory_space=pltpu.VMEM), pl.BlockSpec(memory_space=pl.ANY)
    return pl.pallas_call(
        functools.partial(kernel, Z, C),
        out_shape=jax.ShapeDtypeStruct((J, CH), BF16),
        in_specs=[inside, inside, outside, outside, outside, outside],
        out_specs=inside,
        scratch_shapes=scratch,
        compiler_params=pltpu.CompilerParams(collective_id=0, has_side_effects=True),
        name="conv",
    )(short_taps, skip_gain[None], streams[:, 0], filter_taps, jnp.asarray(tabs), jnp.asarray(dfts))


def local(streams, filter_taps, short_taps, skip_gain, out_weight):
    rows, cols = lax.axis_size("row"), lax.axis_size("col")
    mixed = convolve(rows // 2, cols, streams, filter_taps, short_taps, skip_gain)
    mean_square = jnp.mean(jnp.square(mixed.astype(F32)), axis=-1, keepdims=True)
    product = jnp.dot(mixed, out_weight, preferred_element_type=F32)
    return (product * lax.rsqrt(mean_square + EPSILON)).astype(BF16)[None]


def solution(mesh):
    in_specs = (P(None, None, ("row", "col"), None), P(None, ("row", "col"), None), P(), P(), P())
    return jax.shard_map(local, mesh=mesh, in_specs=in_specs, out_specs=P(None, ("row", "col"), None), check_vma=False)
```

```python
import functools

import jax
import jax.numpy as jnp
import numpy as np
from jax import lax
from jax.experimental import pallas as pl
from jax.experimental.pallas import tpu as pltpu
from jax.sharding import PartitionSpec as P

EPSILON = 1e-06
F32 = jnp.float32
BF16 = jnp.bfloat16
MESH = pl.DeviceIdType.MESH


def tables(freqs, length):
    q = np.arange(freqs, dtype=np.int64)[:, None]
    lane = np.arange(128, dtype=np.int64)[None]

    def circle(numerator, period):
        angles = 2.0 * np.pi * (numerator % period) / period
        return [np.cos(angles), -np.sin(angles)]

    twist = circle((2 * q + 1) * lane, 2 * length)
    fine = circle((2 * q + 1) * lane, 4 * freqs)
    coarse = circle((2 * q + 1) * lane * 128, 4 * freqs)
    tabs = np.stack(twist + fine + coarse).reshape(6, 2, freqs // 2, 128).transpose(1, 0, 2, 3)
    cos, sin = circle(lane.T * lane, 128)
    forward = np.block([[cos, sin], [-sin, cos]])
    back = np.block([[cos, -sin], [sin, cos]])
    pair = np.stack([forward, back])
    high = pair.astype(jnp.bfloat16)
    low = (pair - high.astype(np.float64)).astype(jnp.bfloat16)
    return tabs.astype(np.float32), np.stack([high, low], axis=1)


def dot(a, b):
    return jnp.dot(a, b, preferred_element_type=F32)


def split(x):
    high = x.astype(BF16)
    return high, (x - high.astype(F32)).astype(BF16)


def dot3(x, matrix):
    high, low = split(x)
    return dot(high, matrix[0]) + dot(low, matrix[0]) + dot(high, matrix[1])


def kernel(Z, C, taps_h, skip_h, streams_h, filt_h, tabs_h, dft_h, out, scale,
           taps_w, skip, st, ft, tb, df, he, hr, sm0, sg, fx, fr, gx, gr, tmpf, tmps, zf, zs, xf, xs,
           m1h, m1l, m2, hs, dc, yo, yr, zo, ro, tmpo, xo, rx,
           load, halo_s, halo_r, send, recv, reach):
    J = 128
    CH = Z * C
    S = 2 * CH
    QH = S // 2
    QB = min(256, QH)
    GB = min(128, QH)
    SB = min(128, S)
    ZP, CP = Z + 8, C + 8
    row, col = lax.axis_index("row"), lax.axis_index("col")
    z, core = row // 2, row % 2
    mate = (z * 2 + 1 - core, col)
    block, blocks = row * C + col, 2 * Z * C
    after, before = (block + 1) % blocks, (block + blocks - 1) % blocks
    after_id, before_id = (after // C, after % C), (before // C, before % C)

    loads = [
        pltpu.make_async_copy(streams_h, st, load.at[0]),
        pltpu.make_async_copy(filt_h, ft, load.at[1]),
        pltpu.make_async_copy(tabs_h.at[core], tb, load.at[2]),
        pltpu.make_async_copy(dft_h, df, load.at[3]),
        pltpu.make_async_copy(taps_h, taps_w, load.at[4]),
        pltpu.make_async_copy(skip_h, skip, load.at[5]),
    ]
    for c in loads:
        c.start()

    def z_at(i):
        return (z + Z // 2 + ((i + 1) // 2) * (1 - 2 * (i % 2))) % Z

    def c_at(i):
        return (col + 1 + i) % C

    barrier = pltpu.get_barrier_semaphore()

    def greet_c(i, carry):
        pl.semaphore_signal(barrier, inc=1, device_id=(row, c_at(i)), device_id_type=MESH)
        return carry

    def along_z(k):
        return ((z + k) % Z) * 2 + core, col

    for d in (along_z(1), along_z(Z - 1), mate, after_id, before_id):
        pl.semaphore_signal(barrier, inc=1, device_id=d, device_id_type=MESH)
    lax.fori_loop(0, C - 1, greet_c, 0)

    def tell(k):
        if 2 ** k < Z // 2:
            for d in (along_z(2 ** k), along_z(Z - 2 ** k)):
                pl.semaphore_signal(reach.at[k], inc=1, device_id=d, device_id_type=MESH)

    def hear(k):
        if 2 ** k < Z // 2:
            pl.semaphore_wait(reach.at[k], 2)

    def to_z(src, dst, k, parity=None):
        def pick(i):
            if parity is None:
                return z_at(i)
            odd, sign = (z + parity) % 2, 1 - 2 * (i % 2)
            return (z + Z // 2 + sign * (odd * (1 + 2 * (i // 2)) + (1 - odd) * 2 * ((i + 1) // 2))) % Z

        def body(i, carry):
            t = pick(i)
            pltpu.make_async_remote_copy(
                src_ref=src.at[t], dst_ref=dst, send_sem=send.at[k], recv_sem=recv.at[k],
                device_id=(t * 2 + core, col), device_id_type=MESH).start()
            return carry
        lax.fori_loop(0, Z - 1 if parity is None else Z // 2 - 1 + (z + parity) % 2, body, 0)

    def to_c(src, dst, k):
        def body(i, carry):
            t = c_at(i)
            pltpu.make_async_remote_copy(
                src_ref=src.at[t], dst_ref=dst, send_sem=send.at[k], recv_sem=recv.at[k],
                device_id=(row, t), device_id_type=MESH).start()
            return carry
        lax.fori_loop(0, C - 1, body, 0)

    def await_all(ref, sem):
        pltpu.make_async_copy(ref, ref, sem).wait()

    loads[1].wait()
    for h in range(2):
        fx[:, h] = ft[h].T.astype(BF16).reshape(C, Z, J)
    fr[col] = fx[col]
    loads[0].wait()
    he[...] = jnp.zeros_like(he)
    for i in range(3):
        x = st[i].astype(F32)
        he[0, i:i + 1] = x[J - 1:J]
        he[1, i:i + 1] = x[0:1]

    pl.semaphore_wait(barrier, C - 1 + 5)
    tell(0)

    halos = [
        pltpu.make_async_remote_copy(src_ref=he.at[k], dst_ref=hr.at[k], send_sem=halo_s.at[k],
                                     recv_sem=halo_r.at[k], device_id=d, device_id_type=MESH)
        for k, d in ((0, after_id), (1, before_id))
    ]
    for c in halos:
        c.start()
    to_c(fx, fr.at[col], 0)
    loads[4].wait()
    loads[5].wait()
    hear(0)
    tell(1)
    hear(1)
    tell(2)
    for c in halos:
        c.wait_recv()
    at = lax.broadcasted_iota(jnp.int32, (J, CH), 0)
    smoothed = []
    for i in range(3):
        x = st[i].astype(F32)
        low = jnp.where(block == 0, 0.0, hr[0, i:i + 1])
        high = jnp.where(block == blocks - 1, 0.0, hr[1, i:i + 1])
        low = jnp.where(at == 0, low, pltpu.roll(x, 1, 0))
        high = jnp.where(at == J - 1, high, pltpu.roll(x, J - 1, 0))
        smoothed.append(taps_w[i, 0:1] * low + taps_w[i, 1:2] * x + taps_w[i, 2:3] * high)
    gated = smoothed[2] * smoothed[1]
    gx[...] = gated.T.astype(BF16).reshape(C, Z, J)
    sm0[...] = smoothed[0]
    sg[...] = skip[...] * gated
    gr[col] = gx[col]
    to_c(gx, gr.at[col], 1)
    hear(2)
    tell(3)

    await_all(fr.at[pl.ds(0, C - 1)], recv.at[0])
    for h in range(2):
        for c in range(C):
            tmpf[h, c * ZP:c * ZP + Z] = fr[c, h].astype(F32)
    for h in range(2):
        for t in range(Z):
            zf[t, h] = tmpf[h, pl.ds(t, C, stride=ZP), :].astype(BF16)
    hear(3)
    to_z(zf, xf.at[z, core], 2, 0)
    xf[z, core] = zf[z]
    await_all(gr.at[pl.ds(0, C - 1)], recv.at[1])
    for c in range(C):
        tmps[c * ZP:c * ZP + Z] = gr[c].astype(F32)
    for t in range(Z):
        zs[t] = tmps[pl.ds(t, C, stride=ZP), :].astype(BF16)
    to_z(zs, xs.at[z, core], 3, 0)
    to_z(zf, xf.at[z, core], 2, 1)
    to_z(zs, xs.at[z, core], 3, 1)
    xs[z, core] = zs[z]

    loads[2].wait()
    loads[3].wait()

    def build(g, carry):
        rows = pl.ds(pl.multiple_of(g * GB, GB), GB)
        fine_re, fine_im = tb[2, rows, 0:SB], tb[3, rows, 0:SB]
        for a in range(S // SB):
            coarse_re, coarse_im = tb[4, rows, a:a + 1], tb[5, rows, a:a + 1]
            parts = (coarse_re * fine_re - coarse_im * fine_im, coarse_re * fine_im + coarse_im * fine_re)
            for k, part in enumerate(parts):
                high, low = split(part)
                per = QB // GB
                where = pl.ds(pl.multiple_of((g % per) * GB, GB) + k * QB, GB)
                m1h[g // per, where, a * SB:(a + 1) * SB] = high
                m1l[g // per, where, a * SB:(a + 1) * SB] = low
                flipped = part.T.astype(BF16)
                for n in range(SB // C):
                    tile = a * (SB // C) + n
                    m2[tile % 2, (tile // 2) * C:(tile // 2 + 1) * C, pl.ds(pl.multiple_of(g * GB, GB) + k * QH, GB)] = (
                        flipped[n * C:(n + 1) * C])
        return carry

    lax.fori_loop(0, QH // GB, build, 0)

    def to_mate(src, dst, k):
        pltpu.make_async_remote_copy(
            src_ref=src, dst_ref=dst, send_sem=send.at[k], recv_sem=recv.at[k],
            device_id=mate, device_id_type=MESH).start()

    def twisted(re, im, rows, sign):
        tw_re, tw_im = tb[0, rows], sign * tb[1, rows]
        return re * tw_re - im * tw_im, re * tw_im + im * tw_re

    await_all(xf.at[pl.ds(0, Z - 1), 0], recv.at[2])
    to_mate(xf.at[:, core], xf.at[:, core], 4)
    await_all(xf.at[:, 0], recv.at[4])

    def filter_rows(b, carry):
        rows = pl.ds(pl.multiple_of(b * QB, QB), QB)
        taps = jnp.concatenate([xf[:, :, h].reshape(S, J) for h in range(2)], axis=1)
        p = dot(m1h[b], taps) + dot(m1l[b], taps)
        sign = 1.0 - 2.0 * (lax.broadcasted_iota(jnp.int32, (QB, J), 0) % 2).astype(F32)
        re = p[:QB, :J] - sign * p[QB:, J:]
        im = p[QB:, :J] + sign * p[:QB, J:]
        hs[rows] = dot3(jnp.concatenate(twisted(re, im, rows, 1.0), axis=1), df[0])
        return carry

    lax.fori_loop(0, QH // QB, filter_rows, 0)

    await_all(xs.at[pl.ds(0, Z - 1), 0], recv.at[3])
    to_mate(xs.at[:, core], xs.at[:, core], 5)
    await_all(xs.at[:, 0], recv.at[5])

    def signal_rows(b, carry):
        rows = pl.ds(pl.multiple_of(b * QB, QB), QB)
        p = dot(m1h[b], xs[...].reshape(S, J))
        g = dot3(jnp.concatenate(twisted(p[:QB], p[QB:], rows, 1.0), axis=1), df[0])
        h = hs[rows]
        gre, gim, hre, him = g[:, :J], g[:, J:], h[:, :J], h[:, J:]
        y = dot3(jnp.concatenate([gre * hre - gim * him, gre * him + gim * hre], axis=1), df[1])
        parts = twisted(y[:, :J], y[:, J:], rows, -1.0)
        for k, part in enumerate(parts):
            high, low = split(part * (1.0 / (S * J)))
            where = pl.ds(pl.multiple_of(b * QB, QB) + k * QH, QB)
            dc[where, 0:J] = high
            dc[where, J:2 * J] = low
        return carry

    lax.fori_loop(0, QH // QB, signal_rows, 0)
    other = dot(m2[1 - core], dc[...])
    yo[...] = (other[:, :J] + other[:, J:]).reshape(Z, C, J)
    to_mate(yo, yr, 6)
    own = dot(m2[core], dc[...])
    own = (own[:, :J] + own[:, J:]).reshape(Z, C, J)
    await_all(yr, recv.at[6])
    zo[...] = (own + yr[...]).astype(BF16)
    to_z(zo, ro.at[z], 7)
    ro[z] = zo[z]
    await_all(ro.at[pl.ds(0, Z - 1)], recv.at[7])
    for t in range(Z):
        tmpo[t * CP:t * CP + C] = ro[t].astype(F32)
    for c in range(C):
        xo[c] = tmpo[pl.ds(c, Z, stride=CP), :].astype(BF16)
    to_c(xo, rx.at[col], 8)
    rx[col] = xo[col]
    await_all(rx.at[pl.ds(0, C - 1)], recv.at[8])
    convolved = rx[...].reshape(CH, J).astype(F32).T
    mixed = ((convolved + sg[...]) * sm0[...]).astype(BF16)
    out[...] = mixed
    mean_square = jnp.mean(jnp.square(mixed.astype(F32)), axis=-1, keepdims=True)
    scale[...] = jnp.broadcast_to(lax.rsqrt(mean_square + EPSILON), (J, 128))

    for c in halos:
        c.wait_send()
    for ref, k in ((fx.at[pl.ds(0, C - 1)], 0), (gx.at[pl.ds(0, C - 1)], 1), (zf.at[pl.ds(0, Z - 1)], 2),
                   (zs.at[pl.ds(0, Z - 1)], 3), (xf.at[:, 0], 4), (xs.at[:, 0], 5), (yo, 6),
                   (zo.at[pl.ds(0, Z - 1)], 7), (xo.at[pl.ds(0, C - 1)], 8)):
        await_all(ref, send.at[k])


def convolve(Z, C, streams, filter_taps, short_taps, skip_gain):
    J, CH = 128, Z * C
    S = 2 * CH
    QH = S // 2
    QB = min(256, QH)
    tabs, dfts = tables(S, 2 * S * J)
    vmem = pltpu.VMEM
    scratch = [
        vmem((3, 3, CH), F32),
        vmem((1, CH), F32),
        vmem((3, J, CH), BF16),
        vmem((2, J, CH), F32),
        vmem((6, QH, 128), F32),
        vmem((2, 2, 2 * J, 2 * J), BF16),
        vmem((2, 8, CH), F32),
        vmem((2, 8, CH), F32),
        vmem((J, CH), F32),
        vmem((J, CH), F32),
        vmem((C, 2, Z, J), BF16),
        vmem((C, 2, Z, J), BF16),
        vmem((C, Z, J), BF16),
        vmem((C, Z, J), BF16),
        vmem((2, C * (Z + 8), J), F32),
        vmem((C * (Z + 8), J), F32),
        vmem((Z, 2, C, J), BF16),
        vmem((Z, C, J), BF16),
        vmem((Z, 2, 2, C, J), BF16),
        vmem((Z, 2, C, J), BF16),
        vmem((QH // QB, 2 * QB, S), BF16),
        vmem((QH // QB, 2 * QB, S), BF16),
        vmem((2, S // 2, 2 * QH), BF16),
        vmem((QH, 2 * J), F32),
        vmem((2 * QH, 2 * J), BF16),
        vmem((Z, C, J), F32),
        vmem((Z, C, J), F32),
        vmem((Z, C, J), BF16),
        vmem((Z, C, J), BF16),
        vmem((Z * (C + 8), J), F32),
        vmem((C, Z, J), BF16),
        vmem((C, Z, J), BF16),
        pltpu.SemaphoreType.DMA((6,)),
        pltpu.SemaphoreType.DMA((2,)),
        pltpu.SemaphoreType.DMA((2,)),
        pltpu.SemaphoreType.DMA((9,)),
        pltpu.SemaphoreType.DMA((9,)),
        pltpu.SemaphoreType.REGULAR((4,)),
    ]
    inside, outside = pl.BlockSpec(memory_space=pltpu.VMEM), pl.BlockSpec(memory_space=pltpu.HBM)
    return pl.pallas_call(
        functools.partial(kernel, Z, C),
        out_shape=[jax.ShapeDtypeStruct((J, CH), BF16), jax.ShapeDtypeStruct((J, 128), F32)],
        in_specs=[outside, outside, outside, outside, outside, outside],
        out_specs=[inside, inside],
        scratch_shapes=scratch,
        compiler_params=pltpu.CompilerParams(collective_id=0, has_side_effects=True, vmem_limit_bytes=58 * 2**20),
        name="conv",
    )(short_taps, skip_gain[None], streams[:, 0], filter_taps, jnp.asarray(tabs), jnp.asarray(dfts))


def local(streams, filter_taps, short_taps, skip_gain, out_weight):
    rows, cols = lax.axis_size("row"), lax.axis_size("col")
    mixed, scale = convolve(rows // 2, cols, streams, filter_taps, short_taps, skip_gain)
    product = jnp.dot(mixed, out_weight, preferred_element_type=F32)
    return (product * scale[:, :1]).astype(BF16)[None]


def solution(mesh):
    in_specs = (P(None, None, ("row", "col"), None), P(None, ("row", "col"), None), P(), P(), P())
    return jax.shard_map(local, mesh=mesh, in_specs=in_specs, out_specs=P(None, ("row", "col"), None), check_vma=False)
```

```python
import functools

import jax
import jax.numpy as jnp
import numpy as np
from jax import lax
from jax.experimental import pallas as pl
from jax.experimental.pallas import tpu as pltpu
from jax.sharding import PartitionSpec as P

EPSILON = 1e-06
F32 = jnp.float32
BF16 = jnp.bfloat16
MESH = pl.DeviceIdType.MESH


def tables(freqs, length):
    q = np.arange(freqs, dtype=np.int64)[:, None]
    lane = np.arange(128, dtype=np.int64)[None]

    def circle(numerator, period):
        angles = 2.0 * np.pi * (numerator % period) / period
        return [np.cos(angles), -np.sin(angles)]

    twist = circle((2 * q + 1) * lane, 2 * length)
    fine = circle((2 * q + 1) * lane, 4 * freqs)
    coarse = circle((2 * q + 1) * lane * 128, 4 * freqs)
    tabs = np.stack(twist + fine + coarse).reshape(6, 2, freqs // 2, 128).transpose(1, 0, 2, 3)
    cos, sin = circle(lane.T * lane, 128)
    forward = np.block([[cos, sin], [-sin, cos]])
    back = np.block([[cos, -sin], [sin, cos]])
    pair = np.stack([forward, back])
    high = pair.astype(jnp.bfloat16)
    low = (pair - high.astype(np.float64)).astype(jnp.bfloat16)
    return tabs.astype(np.float32), np.stack([high, low], axis=1)


def dot(a, b):
    return jnp.dot(a, b, preferred_element_type=F32)


def split(x):
    high = x.astype(BF16)
    return high, (x - high.astype(F32)).astype(BF16)


def dot3(x, matrix):
    high, low = split(x)
    return dot(high, matrix[0]) + dot(low, matrix[0]) + dot(high, matrix[1])


def kernel(Z, C, taps_h, skip_h, streams_h, filt_h, tabs_h, dft_h, out, scale,
           taps_w, skip, st, ft, tb, df, he, hr, sm0, sg, fx, fr, gx, gr, tmpf, tmps, zf, zs, xf, xs,
           m1h, m1l, m2, hs, dc, yo, yr, zo, ro, tmpo, xo, rx,
           load, halo_s, halo_r, send, recv, reach):
    J = 128
    CH = Z * C
    S = 2 * CH
    QH = S // 2
    QB = min(256, QH)
    GB = min(128, QH)
    SB = min(128, S)
    ZP, CP = Z + 8, C + 8
    row, col = lax.axis_index("row"), lax.axis_index("col")
    z, core = row // 2, row % 2
    mate = (z * 2 + 1 - core, col)
    block, blocks = row * C + col, 2 * Z * C
    after, before = (block + 1) % blocks, (block + blocks - 1) % blocks
    after_id, before_id = (after // C, after % C), (before // C, before % C)

    loads = [
        pltpu.make_async_copy(streams_h, st, load.at[0]),
        pltpu.make_async_copy(filt_h, ft, load.at[1]),
        pltpu.make_async_copy(tabs_h.at[core], tb, load.at[2]),
        pltpu.make_async_copy(dft_h, df, load.at[3]),
        pltpu.make_async_copy(taps_h, taps_w, load.at[4]),
        pltpu.make_async_copy(skip_h, skip, load.at[5]),
    ]
    def z_at(i):
        return (z + Z // 2 + ((i + 1) // 2) * (1 - 2 * (i % 2))) % Z

    def c_at(i):
        return (col + 1 + (i + 5 * C // 8 - 1) % (C - 1)) % C

    barrier = pltpu.get_barrier_semaphore()

    def greet_c(i, carry):
        pl.semaphore_signal(barrier, inc=1, device_id=(row, c_at(i)), device_id_type=MESH)
        return carry

    def along_z(k):
        return ((z + k) % Z) * 2 + core, col

    for d in (along_z(1), along_z(Z - 1), mate, after_id, before_id):
        pl.semaphore_signal(barrier, inc=1, device_id=d, device_id_type=MESH)
    for k in (1, 0):
        loads[k].start()
    lax.fori_loop(0, C - 1, greet_c, 0, unroll=True)
    for c in loads[2:]:
        c.start()

    def tell(k):
        if 2 ** k < Z // 2:
            for d in (along_z(2 ** k), along_z(Z - 2 ** k)):
                pl.semaphore_signal(reach.at[k], inc=1, device_id=d, device_id_type=MESH)

    def hear(k):
        if 2 ** k < Z // 2:
            pl.semaphore_wait(reach.at[k], 2)

    def to_z(src, dst, k, choose=None):
        def body(i, carry):
            t = z_at(i)

            def go():
                pltpu.make_async_remote_copy(
                    src_ref=src.at[t], dst_ref=dst, send_sem=send.at[k], recv_sem=recv.at[k],
                    device_id=(t * 2 + core, col), device_id_type=MESH).start()

            if choose is None:
                go()
            else:
                pl.when(choose((i + 1) // 2, t))(go)
            return carry
        lax.fori_loop(0, Z - 1, body, 0)

    def near_first(n, t):
        return n >= Z // 4

    def far_first(n, t):
        return n < Z // 4

    def first(n, t):
        return t % 4 != 3

    def last(n, t):
        return t % 4 == 3

    def to_c(src, dst, k):
        def body(i, carry):
            t = c_at(i)
            pltpu.make_async_remote_copy(
                src_ref=src.at[t], dst_ref=dst, send_sem=send.at[k], recv_sem=recv.at[k],
                device_id=(row, t), device_id_type=MESH).start()
            return carry
        lax.fori_loop(0, C - 1, body, 0, unroll=True)

    def await_all(ref, sem):
        pltpu.make_async_copy(ref, ref, sem).wait()

    loads[1].wait()
    for h in range(2):
        fx[:, h] = ft[h].T.astype(BF16).reshape(C, Z, J)
    fr[col] = fx[col]
    loads[0].wait()
    he[...] = jnp.zeros_like(he)
    for i in range(3):
        x = st[i].astype(F32)
        he[0, i:i + 1] = x[J - 1:J]
        he[1, i:i + 1] = x[0:1]

    pl.semaphore_wait(barrier, C - 1 + 5)
    tell(0)

    halos = [
        pltpu.make_async_remote_copy(src_ref=he.at[k], dst_ref=hr.at[k], send_sem=halo_s.at[k],
                                     recv_sem=halo_r.at[k], device_id=d, device_id_type=MESH)
        for k, d in ((0, after_id), (1, before_id))
    ]
    for c in halos:
        c.start()
    to_c(fx, fr.at[col], 0)
    loads[4].wait()
    loads[5].wait()
    hear(0)
    tell(1)
    hear(1)
    tell(2)
    for c in halos:
        c.wait_recv()
    at = lax.broadcasted_iota(jnp.int32, (J, CH), 0)
    smoothed = []
    for i in range(3):
        x = st[i].astype(F32)
        low = jnp.where(block == 0, 0.0, hr[0, i:i + 1])
        high = jnp.where(block == blocks - 1, 0.0, hr[1, i:i + 1])
        low = jnp.where(at == 0, low, pltpu.roll(x, 1, 0))
        high = jnp.where(at == J - 1, high, pltpu.roll(x, J - 1, 0))
        smoothed.append(taps_w[i, 0:1] * low + taps_w[i, 1:2] * x + taps_w[i, 2:3] * high)
    gated = smoothed[2] * smoothed[1]
    gx[...] = gated.T.astype(BF16).reshape(C, Z, J)
    sm0[...] = smoothed[0]
    sg[...] = skip[...] * gated
    gr[col] = gx[col]
    to_c(gx, gr.at[col], 1)
    hear(2)
    tell(3)

    await_all(fr.at[pl.ds(0, C - 1)], recv.at[0])
    for h in range(2):
        for c in range(C):
            tmpf[h, c * ZP:c * ZP + Z] = fr[c, h].astype(F32)
    for h in range(2):
        for t in range(Z):
            zf[t, h] = tmpf[h, pl.ds(t, C, stride=ZP), :].astype(BF16)
    to_z(zf, xf.at[z, core], 2, near_first)
    xf[z, core] = zf[z]
    await_all(gr.at[pl.ds(0, C - 1)], recv.at[1])
    for c in range(C):
        tmps[c * ZP:c * ZP + Z] = gr[c].astype(F32)
    for t in range(Z):
        zs[t] = tmps[pl.ds(t, C, stride=ZP), :].astype(BF16)
    hear(3)
    to_z(zf, xf.at[z, core], 2, far_first)
    for k in range(4):
        to_z(zs, xs.at[z, core], 3, lambda n, t, k=k: t % 4 == k)
    xs[z, core] = zs[z]

    loads[2].wait()
    loads[3].wait()

    def build(g, carry):
        rows = pl.ds(pl.multiple_of(g * GB, GB), GB)
        fine_re, fine_im = tb[2, rows, 0:SB], tb[3, rows, 0:SB]
        for a in range(S // SB):
            coarse_re, coarse_im = tb[4, rows, a:a + 1], tb[5, rows, a:a + 1]
            parts = (coarse_re * fine_re - coarse_im * fine_im, coarse_re * fine_im + coarse_im * fine_re)
            for k, part in enumerate(parts):
                high, low = split(part)
                per = QB // GB
                where = pl.ds(pl.multiple_of((g % per) * GB, GB) + k * QB, GB)
                m1h[g // per, where, a * SB:(a + 1) * SB] = high
                m1l[g // per, where, a * SB:(a + 1) * SB] = low
                flipped = part.T.astype(BF16)
                for n in range(SB // C):
                    tile = a * (SB // C) + n
                    m2[tile % 2, (tile // 2) * C:(tile // 2 + 1) * C, pl.ds(pl.multiple_of(g * GB, GB) + k * QH, GB)] = (
                        flipped[n * C:(n + 1) * C])
        return carry

    lax.fori_loop(0, QH // GB, build, 0)

    def to_mate(src, dst, k):
        pltpu.make_async_remote_copy(
            src_ref=src, dst_ref=dst, send_sem=send.at[k], recv_sem=recv.at[k],
            device_id=mate, device_id_type=MESH).start()

    def twisted(re, im, rows, sign):
        tw_re, tw_im = tb[0, rows], sign * tb[1, rows]
        return re * tw_re - im * tw_im, re * tw_im + im * tw_re

    await_all(xf.at[pl.ds(0, Z - 1), 0], recv.at[2])
    to_mate(xf.at[:, core], xf.at[:, core], 4)
    await_all(xf.at[:, 0], recv.at[4])

    def filter_rows(b, carry):
        rows = pl.ds(pl.multiple_of(b * QB, QB), QB)
        taps = jnp.concatenate([xf[:, :, h].reshape(S, J) for h in range(2)], axis=1)
        p = dot(m1h[b], taps) + dot(m1l[b], taps)
        sign = 1.0 - 2.0 * (lax.broadcasted_iota(jnp.int32, (QB, J), 0) % 2).astype(F32)
        re = p[:QB, :J] - sign * p[QB:, J:]
        im = p[QB:, :J] + sign * p[:QB, J:]
        hs[rows] = dot3(jnp.concatenate(twisted(re, im, rows, 1.0), axis=1), df[0])
        return carry

    lax.fori_loop(0, QH // QB, filter_rows, 0)

    await_all(xs.at[pl.ds(0, Z - 1), 0], recv.at[3])
    to_mate(xs.at[:, core], xs.at[:, core], 5)
    await_all(xs.at[:, 0], recv.at[5])

    def signal_rows(b, carry):
        rows = pl.ds(pl.multiple_of(b * QB, QB), QB)
        p = dot(m1h[b], xs[...].reshape(S, J))
        g = dot3(jnp.concatenate(twisted(p[:QB], p[QB:], rows, 1.0), axis=1), df[0])
        h = hs[rows]
        gre, gim, hre, him = g[:, :J], g[:, J:], h[:, :J], h[:, J:]
        y = dot3(jnp.concatenate([gre * hre - gim * him, gre * him + gim * hre], axis=1), df[1])
        parts = twisted(y[:, :J], y[:, J:], rows, -1.0)
        for k, part in enumerate(parts):
            high, low = split(part * (1.0 / (S * J)))
            where = pl.ds(pl.multiple_of(b * QB, QB) + k * QH, QB)
            dc[where, 0:J] = high
            dc[where, J:2 * J] = low
        return carry

    lax.fori_loop(0, QH // QB, signal_rows, 0, unroll=True)
    other = dot(m2[1 - core], dc[...])
    yo[...] = (other[:, :J] + other[:, J:]).reshape(Z, C, J)
    to_mate(yo, yr, 6)
    own = dot(m2[core], dc[...])
    own = (own[:, :J] + own[:, J:]).reshape(Z, C, J)
    await_all(yr, recv.at[6])
    zo[...] = (own + yr[...]).astype(BF16)
    to_z(zo, ro.at[z], 7)
    ro[z] = zo[z]
    await_all(ro.at[pl.ds(0, Z - 1)], recv.at[7])
    for t in range(Z):
        tmpo[t * CP:t * CP + C] = ro[t].astype(F32)
    for c in range(C):
        xo[c] = tmpo[pl.ds(c, Z, stride=CP), :].astype(BF16)
    to_c(xo, rx.at[col], 8)
    rx[col] = xo[col]
    await_all(rx.at[pl.ds(0, C - 1)], recv.at[8])
    convolved = rx[...].reshape(CH, J).astype(F32).T
    mixed = ((convolved + sg[...]) * sm0[...]).astype(BF16)
    out[...] = mixed
    mean_square = jnp.mean(jnp.square(mixed.astype(F32)), axis=-1, keepdims=True)
    scale[...] = jnp.broadcast_to(lax.rsqrt(mean_square + EPSILON), (J, J)).T[0:1]

    for c in halos:
        c.wait_send()
    for ref, k in ((fx.at[pl.ds(0, C - 1)], 0), (gx.at[pl.ds(0, C - 1)], 1), (zf.at[pl.ds(0, Z - 1)], 2),
                   (zs.at[pl.ds(0, Z - 1)], 3), (xf.at[:, 0], 4), (xs.at[:, 0], 5), (yo, 6),
                   (zo.at[pl.ds(0, Z - 1)], 7), (xo.at[pl.ds(0, C - 1)], 8)):
        await_all(ref, send.at[k])


def convolve(Z, C, streams, filter_taps, short_taps, skip_gain):
    J, CH = 128, Z * C
    S = 2 * CH
    QH = S // 2
    QB = min(256, QH)
    tabs, dfts = tables(S, 2 * S * J)
    vmem = pltpu.VMEM
    scratch = [
        vmem((3, 3, CH), F32),
        vmem((1, CH), F32),
        vmem((3, J, CH), BF16),
        vmem((2, J, CH), F32),
        vmem((6, QH, 128), F32),
        vmem((2, 2, 2 * J, 2 * J), BF16),
        vmem((2, 8, CH), F32),
        vmem((2, 8, CH), F32),
        vmem((J, CH), F32),
        vmem((J, CH), F32),
        vmem((C, 2, Z, J), BF16),
        vmem((C, 2, Z, J), BF16),
        vmem((C, Z, J), BF16),
        vmem((C, Z, J), BF16),
        vmem((2, C * (Z + 8), J), F32),
        vmem((C * (Z + 8), J), F32),
        vmem((Z, 2, C, J), BF16),
        vmem((Z, C, J), BF16),
        vmem((Z, 2, 2, C, J), BF16),
        vmem((Z, 2, C, J), BF16),
        vmem((QH // QB, 2 * QB, S), BF16),
        vmem((QH // QB, 2 * QB, S), BF16),
        vmem((2, S // 2, 2 * QH), BF16),
        vmem((QH, 2 * J), F32),
        vmem((2 * QH, 2 * J), BF16),
        vmem((Z, C, J), F32),
        vmem((Z, C, J), F32),
        vmem((Z, C, J), BF16),
        vmem((Z, C, J), BF16),
        vmem((Z * (C + 8), J), F32),
        vmem((C, Z, J), BF16),
        vmem((C, Z, J), BF16),
        pltpu.SemaphoreType.DMA((6,)),
        pltpu.SemaphoreType.DMA((2,)),
        pltpu.SemaphoreType.DMA((2,)),
        pltpu.SemaphoreType.DMA((9,)),
        pltpu.SemaphoreType.DMA((9,)),
        pltpu.SemaphoreType.REGULAR((4,)),
    ]
    inside, outside = pl.BlockSpec(memory_space=pltpu.VMEM), pl.BlockSpec(memory_space=pltpu.HBM)
    return pl.pallas_call(
        functools.partial(kernel, Z, C),
        out_shape=[jax.ShapeDtypeStruct((J, CH), BF16), jax.ShapeDtypeStruct((1, J), F32)],
        in_specs=[outside] * 6,
        out_specs=[inside, inside],
        scratch_shapes=scratch,
        compiler_params=pltpu.CompilerParams(collective_id=0, has_side_effects=True, vmem_limit_bytes=429 * 2**17),
        name="conv",
    )(short_taps, skip_gain[None], streams[:, 0], filter_taps, jnp.asarray(tabs), jnp.asarray(dfts))


def local(streams, filter_taps, short_taps, skip_gain, out_weight):
    rows, cols = lax.axis_size("row"), lax.axis_size("col")
    mixed, scale = convolve(rows // 2, cols, streams, filter_taps, short_taps, skip_gain)
    product = jnp.dot(mixed, out_weight, preferred_element_type=F32)
    return (product * scale[0][:, None]).astype(BF16)[None]


def solution(mesh):
    in_specs = (P(None, None, ("row", "col"), None), P(None, ("row", "col"), None), P(), P(), P())
    return jax.shard_map(local, mesh=mesh, in_specs=in_specs, out_specs=P(None, ("row", "col"), None), check_vma=False)
```

```python
import functools

import jax
import jax.numpy as jnp
import numpy as np
from jax import lax
from jax.experimental import pallas as pl
from jax.experimental.pallas import tpu as pltpu
from jax.sharding import PartitionSpec as P

EPSILON = 1e-06
F32 = jnp.float32
BF16 = jnp.bfloat16
MESH = pl.DeviceIdType.MESH


def tables(freqs, length, tile):
    direct = np.arange(freqs // 2, dtype=np.int64).reshape(2, -1)
    q = np.concatenate([direct, freqs - 1 - direct], axis=1).reshape(-1, 1)
    lane = np.arange(128, dtype=np.int64)[None]

    def circle(numerator, period):
        angles = 2.0 * np.pi * (numerator % period) / period
        return [np.cos(angles), -np.sin(angles)]

    per, half = freqs // 4, tile // 2
    block = min(128, per)
    count = per // block
    steps = 2 * tile * (lane // half) + 2 * (lane % half)
    starts = 2 * tile * (lane % count) * (block // half) + tile * (lane // count % 2) + lane // (2 * count)
    twist = circle((2 * q + 1) * lane, 2 * length)
    fine = circle((2 * q + 1) * steps, 4 * freqs)
    coarse = circle((2 * q + 1) * starts, 4 * freqs)
    tabs = np.stack(twist + fine + coarse).reshape(6, 2, freqs // 2, 128).transpose(1, 0, 2, 3)
    cos, sin = circle(lane.T * lane, 128)
    forward = np.block([[cos, sin], [-sin, cos]])
    back = np.block([[cos, -sin], [sin, cos]])
    pair = np.stack([forward, back])
    high = pair.astype(jnp.bfloat16)
    low = (pair - high.astype(np.float64)).astype(jnp.bfloat16)
    return tabs.astype(np.float32), np.stack([high, low], axis=1)


def dot(a, b):
    return jnp.dot(a, b, preferred_element_type=F32)


def split(x):
    high = x.astype(BF16)
    return high, (x - high.astype(F32)).astype(BF16)


def dot3(x, matrix):
    high, low = split(x)
    return dot(high, matrix[0]) + dot(low, matrix[0]) + dot(high, matrix[1])


def kernel(Z, C, taps_h, skip_h, streams_h, filt_h, tabs_h, dft_h, out, scale,
           taps_w, skip, st, ft, tb, df, he, hr, sm0, sg, fx, fr, gx, gr, tmpf, tmps, zf, zs, xf, xs,
           m1h, m1l, m2, ps, hs, dc, yo, yr, zo, ro, tmpo, xo, rx,
           load, halo_s, halo_r, send, recv, reach):
    J = 128
    CH = Z * C
    S = 2 * CH
    QH = S // 2
    QD, C2 = QH // 2, C // 2
    PP = Z * C2
    GB = min(128, QD)
    SB = min(128, PP)
    ZP, CP = Z + 8, C + 8
    row, col = lax.axis_index("row"), lax.axis_index("col")
    z, core = row // 2, row % 2
    mate = (z * 2 + 1 - core, col)
    block, blocks = row * C + col, 2 * Z * C
    after, before = (block + 1) % blocks, (block + blocks - 1) % blocks
    after_id, before_id = (after // C, after % C), (before // C, before % C)

    loads = [
        pltpu.make_async_copy(streams_h, st, load.at[0]),
        pltpu.make_async_copy(filt_h, ft, load.at[1]),
        pltpu.make_async_copy(tabs_h.at[core], tb, load.at[2]),
        pltpu.make_async_copy(dft_h, df, load.at[3]),
        pltpu.make_async_copy(taps_h, taps_w, load.at[4]),
        pltpu.make_async_copy(skip_h, skip, load.at[5]),
    ]
    def z_at(i):
        return (z + Z // 2 + ((i + 1) // 2) * (1 - 2 * (i % 2))) % Z

    def c_at(i):
        return (col + 1 + (i + 5 * C // 8 - 1) % (C - 1)) % C

    barrier = pltpu.get_barrier_semaphore()

    def greet_c(i, carry):
        pl.semaphore_signal(barrier, inc=1, device_id=(row, c_at(i)), device_id_type=MESH)
        return carry

    def along_z(k):
        return ((z + k) % Z) * 2 + core, col

    for d in (along_z(1), along_z(Z - 1), mate, after_id, before_id):
        pl.semaphore_signal(barrier, inc=1, device_id=d, device_id_type=MESH)
    for k in (1, 0):
        loads[k].start()
    lax.fori_loop(0, C - 1, greet_c, 0, unroll=True)
    for c in loads[2:]:
        c.start()

    def tell(k):
        if 2 ** k < Z // 2:
            for d in (along_z(2 ** k), along_z(Z - 2 ** k)):
                pl.semaphore_signal(reach.at[k], inc=1, device_id=d, device_id_type=MESH)

    def hear(k):
        if 2 ** k < Z // 2:
            pl.semaphore_wait(reach.at[k], 2)

    def to_z(src, dst, k, choose=None):
        def body(i, carry):
            t = z_at(i)

            def go():
                pltpu.make_async_remote_copy(
                    src_ref=src.at[t], dst_ref=dst, send_sem=send.at[k], recv_sem=recv.at[k],
                    device_id=(t * 2 + core, col), device_id_type=MESH).start()

            if choose is None:
                go()
            else:
                pl.when(choose((i + 1) // 2, t))(go)
            return carry
        lax.fori_loop(0, Z - 1, body, 0)

    def near_first(n, t):
        return n >= Z // 4

    def far_first(n, t):
        return n < Z // 4

    def first(n, t):
        return t % 4 != 3

    def last(n, t):
        return t % 4 == 3

    def to_c(src, dst, k):
        def body(i, carry):
            t = c_at(i)
            pltpu.make_async_remote_copy(
                src_ref=src.at[t], dst_ref=dst, send_sem=send.at[k], recv_sem=recv.at[k],
                device_id=(row, t), device_id_type=MESH).start()
            return carry
        lax.fori_loop(0, C - 1, body, 0, unroll=True)

    def seat(c):
        return c % 2 * C2 + c // 2

    def await_all(ref, sem):
        pltpu.make_async_copy(ref, ref, sem).wait()

    loads[1].wait()
    for h in range(2):
        fx[:, h] = ft[h].T.astype(BF16).reshape(C, Z, J)
    fr[col] = fx[col]
    loads[0].wait()
    he[...] = jnp.zeros_like(he)
    for i in range(3):
        x = st[i].astype(F32)
        he[0, i:i + 1] = x[J - 1:J]
        he[1, i:i + 1] = x[0:1]

    pl.semaphore_wait(barrier, C - 1 + 5)
    tell(0)

    halos = [
        pltpu.make_async_remote_copy(src_ref=he.at[k], dst_ref=hr.at[k], send_sem=halo_s.at[k],
                                     recv_sem=halo_r.at[k], device_id=d, device_id_type=MESH)
        for k, d in ((0, after_id), (1, before_id))
    ]
    for c in halos:
        c.start()
    to_c(fx, fr.at[col], 0)
    loads[4].wait()
    loads[5].wait()
    hear(0)
    tell(1)
    hear(1)
    tell(2)
    for c in halos:
        c.wait_recv()
    at = lax.broadcasted_iota(jnp.int32, (J, CH), 0)
    smoothed = []
    for i in range(3):
        x = st[i].astype(F32)
        low = jnp.where(block == 0, 0.0, hr[0, i:i + 1])
        high = jnp.where(block == blocks - 1, 0.0, hr[1, i:i + 1])
        low = jnp.where(at == 0, low, pltpu.roll(x, 1, 0))
        high = jnp.where(at == J - 1, high, pltpu.roll(x, J - 1, 0))
        smoothed.append(taps_w[i, 0:1] * low + taps_w[i, 1:2] * x + taps_w[i, 2:3] * high)
    gated = smoothed[2] * smoothed[1]
    gx[...] = gated.T.astype(BF16).reshape(C, Z, J)
    sm0[...] = smoothed[0]
    sg[...] = skip[...] * gated
    gr[col] = gx[col]
    to_c(gx, gr.at[col], 1)
    hear(2)
    tell(3)

    await_all(fr.at[pl.ds(0, C - 1)], recv.at[0])
    for h in range(2):
        for c in range(C):
            tmpf[h, seat(c) * ZP:seat(c) * ZP + Z] = fr[c, h].astype(F32)
    for h in range(2):
        for t in range(Z):
            zf[t, h] = tmpf[h, pl.ds(t, C, stride=ZP), :].astype(BF16)
    to_z(zf, xf.at[core, z], 2, near_first)
    xf[core, z] = zf[z]
    await_all(gr.at[pl.ds(0, C - 1)], recv.at[1])
    for c in range(C):
        tmps[seat(c) * ZP:seat(c) * ZP + Z] = gr[c].astype(F32)
    for t in range(Z):
        zs[t] = tmps[pl.ds(t, C, stride=ZP), :].astype(BF16)
    hear(3)
    to_z(zf, xf.at[core, z], 2, far_first)
    for k in range(4):
        to_z(zs, xs.at[core, z], 3, lambda n, t, k=k: t % 4 == k)
    xs[core, z] = zs[z]

    loads[2].wait()
    loads[3].wait()

    def build(g, carry):
        at_q = pl.multiple_of(g * GB, GB)
        rows = pl.ds(at_q, GB)
        fine_re, fine_im = tb[2, rows, 0:SB], tb[3, rows, 0:SB]
        for a in range(S // SB):
            coarse_re, coarse_im = tb[4, rows, a:a + 1], tb[5, rows, a:a + 1]
            parts = (coarse_re * fine_re - coarse_im * fine_im, coarse_re * fine_im + coarse_im * fine_re)
            for k, part in enumerate(parts):
                high, low = split(part)
                m1h[pl.ds(at_q + k * QD, GB), a * SB:(a + 1) * SB] = high
                m1l[pl.ds(at_q + k * QD, GB), a * SB:(a + 1) * SB] = low
                m2[a * SB:(a + 1) * SB, pl.ds(at_q + k * QD, GB)] = part.T.astype(BF16)
        return carry

    lax.fori_loop(0, QD // GB, build, 0)

    def to_mate(src, dst, k):
        pltpu.make_async_remote_copy(
            src_ref=src, dst_ref=dst, send_sem=send.at[k], recv_sem=recv.at[k],
            device_id=mate, device_id_type=MESH).start()

    def twisted(re, im, rows, sign):
        tw_re, tw_im = tb[0, rows], sign * tb[1, rows]
        return re * tw_re - im * tw_im, re * tw_im + im * tw_re

    def both_halves(even, odd):
        ere, eim, ore, oim = even[:QD], even[QD:], odd[:QD], odd[QD:]
        return (ere + ore, eim + oim), (ere - ore, oim - eim)

    halves = (slice(0, QD), slice(QD, QH))

    await_all(xf.at[0, pl.ds(0, Z - 1)], recv.at[2])
    to_mate(xf.at[core], xf.at[core], 4)
    await_all(xf.at[0], recv.at[4])
    sums = []
    for k in range(2):
        taps = jnp.concatenate([xf[:, :, h, k * C2:(k + 1) * C2].reshape(2 * PP, J) for h in range(2)], axis=1)
        cols = slice(k * 2 * PP, (k + 1) * 2 * PP)
        sums.append(dot(m1h[:, cols], taps) + dot(m1l[:, cols], taps))
    sign = 1.0 - 2.0 * (lax.broadcasted_iota(jnp.int32, (QD, J), 0) % 2).astype(F32)
    for rows, (re, im), flip in zip(halves, both_halves(*sums), (sign, -sign)):
        re, im = re[:, :J] - flip * im[:, J:], im[:, :J] + flip * re[:, J:]
        hs[rows] = dot3(jnp.concatenate(twisted(re, im, rows, 1.0), axis=1), df[0])

    await_all(xs.at[0, pl.ds(0, Z - 1)], recv.at[3])
    to_mate(xs.at[core], xs.at[core], 5)

    def partial(k, who):
        cols = pl.ds(pl.multiple_of(k * 2 * PP + who * PP, PP), PP)
        return dot(m1h[:, cols], xs[who, :, k * C2:(k + 1) * C2].reshape(PP, J))

    for k in range(2):
        ps[k] = partial(k, core)
    await_all(xs.at[0], recv.at[5])
    sums = [ps[k] + partial(k, 1 - core) for k in range(2)]
    back = []
    for rows, (re, im) in zip(halves, both_halves(*sums)):
        g = dot3(jnp.concatenate(twisted(re, im, rows, 1.0), axis=1), df[0])
        h = hs[rows]
        gre, gim, hre, him = g[:, :J], g[:, J:], h[:, :J], h[:, J:]
        y = dot3(jnp.concatenate([gre * hre - gim * him, gre * him + gim * hre], axis=1), df[1])
        back.append([part * (1.0 / (S * J)) for part in twisted(y[:, :J], y[:, J:], rows, -1.0)])
    (dre, dim), (mre, mim) = back
    for k, parts in enumerate(((dre + mre, dim - mim), (dre - mre, dim + mim))):
        for n, part in enumerate(parts):
            high, low = split(part)
            dc[k, n * QD:(n + 1) * QD, 0:J] = high
            dc[k, n * QD:(n + 1) * QD, J:2 * J] = low

    def positions(k, who):
        y = dot(m2[pl.ds(pl.multiple_of(k * 2 * PP + who * PP, PP), PP), :], dc[k])
        return (y[:, :J] + y[:, J:]).reshape(Z, C2, J)

    for k in range(2):
        yo[:, k * C2:(k + 1) * C2] = positions(k, 1 - core)
    to_mate(yo, yr, 6)
    own = [positions(k, core) for k in range(2)]
    await_all(yr, recv.at[6])
    zo[...] = (jnp.concatenate(own, axis=1) + yr[...]).astype(BF16)
    to_z(zo, ro.at[z], 7)
    ro[z] = zo[z]
    await_all(ro.at[pl.ds(0, Z - 1)], recv.at[7])
    for t in range(Z):
        tmpo[t * CP:t * CP + C] = ro[t].astype(F32)
    for c in range(C):
        xo[c] = tmpo[pl.ds(seat(c), Z, stride=CP), :].astype(BF16)
    to_c(xo, rx.at[col], 8)
    rx[col] = xo[col]
    await_all(rx.at[pl.ds(0, C - 1)], recv.at[8])
    convolved = rx[...].reshape(CH, J).astype(F32).T
    mixed = ((convolved + sg[...]) * sm0[...]).astype(BF16)
    out[...] = mixed
    mean_square = jnp.mean(jnp.square(mixed.astype(F32)), axis=-1, keepdims=True)
    scale[...] = jnp.broadcast_to(lax.rsqrt(mean_square + EPSILON), (J, J)).T[0:1]

    for c in halos:
        c.wait_send()
    for ref, k in ((fx.at[pl.ds(0, C - 1)], 0), (gx.at[pl.ds(0, C - 1)], 1), (zf.at[pl.ds(0, Z - 1)], 2),
                   (zs.at[pl.ds(0, Z - 1)], 3), (xf.at[0], 4), (xs.at[0], 5), (yo, 6),
                   (zo.at[pl.ds(0, Z - 1)], 7), (xo.at[pl.ds(0, C - 1)], 8)):
        await_all(ref, send.at[k])


def convolve(Z, C, streams, filter_taps, short_taps, skip_gain):
    J, CH = 128, Z * C
    S = 2 * CH
    QH = S // 2
    tabs, dfts = tables(S, 2 * S * J, C)
    vmem = pltpu.VMEM
    scratch = [
        vmem((3, 3, CH), F32),
        vmem((1, CH), F32),
        vmem((3, J, CH), BF16),
        vmem((2, J, CH), F32),
        vmem((6, QH, 128), F32),
        vmem((2, 2, 2 * J, 2 * J), BF16),
        vmem((2, 8, CH), F32),
        vmem((2, 8, CH), F32),
        vmem((J, CH), F32),
        vmem((J, CH), F32),
        vmem((C, 2, Z, J), BF16),
        vmem((C, 2, Z, J), BF16),
        vmem((C, Z, J), BF16),
        vmem((C, Z, J), BF16),
        vmem((2, C * (Z + 8), J), F32),
        vmem((C * (Z + 8), J), F32),
        vmem((Z, 2, C, J), BF16),
        vmem((Z, C, J), BF16),
        vmem((2, Z, 2, C, J), BF16),
        vmem((2, Z, C, J), BF16),
        vmem((QH, S), BF16),
        vmem((QH, S), BF16),
        vmem((S, QH), BF16),
        vmem((2, QH, J), F32),
        vmem((QH, 2 * J), F32),
        vmem((2, QH, 2 * J), BF16),
        vmem((Z, C, J), F32),
        vmem((Z, C, J), F32),
        vmem((Z, C, J), BF16),
        vmem((Z, C, J), BF16),
        vmem((Z * (C + 8), J), F32),
        vmem((C, Z, J), BF16),
        vmem((C, Z, J), BF16),
        pltpu.SemaphoreType.DMA((6,)),
        pltpu.SemaphoreType.DMA((2,)),
        pltpu.SemaphoreType.DMA((2,)),
        pltpu.SemaphoreType.DMA((9,)),
        pltpu.SemaphoreType.DMA((9,)),
        pltpu.SemaphoreType.REGULAR((4,)),
    ]
    inside, outside = pl.BlockSpec(memory_space=pltpu.VMEM), pl.BlockSpec(memory_space=pltpu.HBM)
    return pl.pallas_call(
        functools.partial(kernel, Z, C),
        out_shape=[jax.ShapeDtypeStruct((J, CH), BF16), jax.ShapeDtypeStruct((1, J), F32)],
        in_specs=[outside] * 6,
        out_specs=[inside, inside],
        scratch_shapes=scratch,
        compiler_params=pltpu.CompilerParams(collective_id=0, has_side_effects=True, vmem_limit_bytes=429 * 2**17),
        name="conv",
    )(short_taps, skip_gain[None], streams[:, 0], filter_taps, jnp.asarray(tabs), jnp.asarray(dfts))


def local(streams, filter_taps, short_taps, skip_gain, out_weight):
    rows, cols = lax.axis_size("row"), lax.axis_size("col")
    mixed, scale = convolve(rows // 2, cols, streams, filter_taps, short_taps, skip_gain)
    product = jnp.dot(mixed, out_weight, preferred_element_type=F32)
    return (product * scale[0][:, None]).astype(BF16)[None]


def solution(mesh):
    in_specs = (P(None, None, ("row", "col"), None), P(None, ("row", "col"), None), P(), P(), P())
    return jax.shard_map(local, mesh=mesh, in_specs=in_specs, out_specs=P(None, ("row", "col"), None), check_vma=False)
```
